32 devices in a mesh: fs: 8 (over z, x), tp: 4 (over y, core).
Axes of the slice: x: 2, y: 2, z: 4, core: 2. Of those that a mesh axis runs over, the one named last changes fastest.
Arguments:
- tokens: bfloat16 [768, 4096], P('tp'), may hold values from -6 to 6
- norm_gain: float32 [4096], P('fs'), may hold values from 0.1 to 1.9
- gate_trained: float32 [4096, 11264], P('fs', 'tp'), may hold values from -0.09375 to 0.09375
- up_trained: float32 [4096, 11264], P('fs', 'tp'), may hold values from -0.09375 to 0.09375
- down_trained: float32 [11264, 4096], P('fs', 'tp'), may hold values from -0.078125 to 0.078125
Outputs:
- gate_sampler: bfloat16 [4096, 11264], P(None, 'fs')
- up_sampler: bfloat16 [4096, 11264], P(None, 'fs')
- down_sampler: bfloat16 [11264, 4096], P('fs')
- mixed_out: bfloat16 [768, 4096], P('tp', 'fs')
The draws below stay inside these ranges and needn't reach their ends.
All inputs are finite; a program needn't handle non-finite values.
Results may differ from the reference program's by a relative error of at most 0.0082.
Values may be sent and summed in bfloat16 or wider, within the bound.
A program may use at most 128 MiB of HBM per device.

```python
import jax
import jax.numpy as jnp
from jax import lax

D = 4096
FF = 11264
TOKENS = 768


def spiked(entries, own_key, source, target, shards_of, factor):
    def block_of(axis_at):
        return (jnp.arange(entries.shape[axis_at]) // (entries.shape[axis_at] // shards_of)).reshape((-1,) + (1,) * (entries.ndim - 1 - axis_at))

    first = jax.random.permutation(own_key, shards_of)[block_of(target)]
    second = (block_of(target) + shards_of // 2) % shards_of
    return jnp.where((block_of(source) == first) | (block_of(source) == second), factor * entries, entries)


def shard_levels(rng, dims, shards, least, largest):
    loudness, own = 1.0, jax.random.fold_in(rng, 6)
    for dim, blocks in shards:
        steps = jnp.exp(jax.random.uniform(jax.random.fold_in(own, dim), (blocks,), jnp.float32, least / len(shards), largest / len(shards)))
        loudness = loudness * jnp.repeat(steps, dims[dim] // blocks).reshape([-1 if axis == dim else 1 for axis in range(len(dims))])
    return loudness


def gaussian(own_key, shape, scale, limit, cuts=(), kind=jnp.bfloat16):
    array = scale * jax.random.normal(own_key, shape, jnp.float32)
    if cuts:
        array = array * shard_levels(own_key, shape, cuts, -0.22, 0.18)
    return jnp.clip(array, -limit, limit).astype(kind)


def gaussian_with(rng, shape, scale, reach, split, heavy, held_as=jnp.bfloat16):
    values = scale * jax.random.normal(rng, shape, jnp.float32)
    if split:
        values = values * shard_levels(rng, shape, split, -0.22, 0.18)
    return jnp.clip(spiked(values, jax.random.fold_in(rng, 3), *heavy), -reach, reach).astype(held_as)


def setup_inputs(seed: int = 0) -> dict:
    key_list = jax.random.split(jax.random.key(seed), 6)
    tokens = gaussian(key_list[0], (TOKENS, D), 1.0, 6.0, ((0, 4),))
    norm_gain = jnp.clip(1.0 + 0.18 * jax.random.normal(key_list[1], (D,), jnp.float32), 0.1, 1.9)
    gate_trained = gaussian(key_list[2], (D, FF), D ** -0.5, 0.09375, ((0, 8), (1, 4)), jnp.float32)
    up_trained = gaussian(key_list[3], (D, FF), D ** -0.5, 0.09375, ((0, 8), (1, 4)), jnp.float32)
    down_trained = gaussian_with(key_list[4], (FF, D), FF ** -0.5, 0.078125, ((0, 8), (1, 4)), (0, 1, 8, 2.0), jnp.float32)
    return {"tokens": tokens, "norm_gain": norm_gain, "gate_trained": gate_trained, "up_trained": up_trained, "down_trained": down_trained}


def reference(tokens, norm_gain, gate_trained, up_trained, down_trained):
    gate_sampler = (norm_gain[:, None] * gate_trained).astype(jnp.bfloat16)
    up_sampler = (norm_gain[:, None] * up_trained).astype(jnp.bfloat16)
    down_sampler = down_trained.astype(jnp.bfloat16)
    as_float = tokens.astype(jnp.float32)
    normed = (as_float * jax.lax.rsqrt(lax.optimization_barrier(jnp.mean(as_float * as_float, axis=-1, keepdims=True)) + 1e-06)).astype(jnp.bfloat16)
    gate_act = jnp.dot(normed, gate_sampler, preferred_element_type=jnp.float32)
    up_act = jnp.dot(normed, up_sampler, preferred_element_type=jnp.float32)
    hidden = (jax.nn.silu(gate_act) * up_act).astype(jnp.bfloat16)
    mixed_out = jnp.dot(hidden, down_sampler, preferred_element_type=jnp.float32).astype(jnp.bfloat16)
    return (gate_sampler, up_sampler, down_sampler, mixed_out)
```

```python
import functools

import jax
import jax.numpy as jnp
from jax import lax
from jax.experimental import pallas as pl
from jax.experimental.pallas import tpu as pltpu
from jax.sharding import PartitionSpec as P

MESH = pl.DeviceIdType.MESH


def spread_kernel(
    fs_count, tp_count, single, src_ref, down_ref, gate_ref, up_ref, down_out_ref, stage_ref,
    swap_send, swap_recv, out_send, out_recv, core_send, core_recv, cross_send, cross_recv,
    last_send, last_recv, down_send, down_recv, local_sem,
):
    blocks, mats, rows, _ = src_ref.shape
    down_cols = down_ref.shape[1]
    f = lax.axis_index("fs")
    t = lax.axis_index("tp")
    plane, core = t // 2, t % 2
    across = plane * -2 + 2 + core
    partner = plane * 2 + 1 - core
    outs = (gate_ref, up_ref)
    pieces = ((0, single), (single, single), (2 * single, rows - 2 * single))
    first, second, rest = pieces

    def remote(src, dst, send, recv, to):
        return pltpu.make_async_remote_copy(
            src_ref=src, dst_ref=dst, send_sem=send, recv_sem=recv, device_id=to, device_id_type=MESH
        )

    def place(ref, source, start, size):
        return ref.at[pl.ds(pl.multiple_of(source * rows + start, 16), size), :]

    swaps = []
    for p, (start, size) in enumerate((second, rest)):
        for j in range(blocks):
            for m in range(mats):
                k = (p * blocks + j) * mats + m
                cut = pl.ds(start, size)
                c = remote(
                    src_ref.at[j, m, cut, :], stage_ref.at[j, m, cut, :],
                    swap_send.at[k], swap_recv.at[k], (f, across),
                )
                c.start()
                swaps.append((c, p, j, m))

    sends = []

    def to_owner(ref, owner, j, m, p, start, size):
        k = len(sends)
        source = ref.at[j, m, pl.ds(start, size), :]
        landing = place(outs[m], f, start, size)
        local = jnp.logical_and(owner == f, core == m)
        there = remote(source, landing, out_send.at[k], out_recv.at[f, p], (owner, plane * 2 + m))

        @pl.when(local)
        def _():
            pltpu.make_async_copy(source, landing, out_recv.at[f, p]).start()

        @pl.when(jnp.logical_not(local))
        def _():
            there.start()

        sends.append((there, local))

    for p, (start, size) in enumerate((first, rest)):
        for j in range(blocks):
            for m in range(mats):
                to_owner(src_ref, t * blocks + j, j, m, p, start, size)

    def down_at(which):
        return down_out_ref.at[:, pl.ds(pl.multiple_of(which * down_cols, 128), down_cols)]

    down_cross = remote(down_ref, down_at(t), down_send.at[0], down_recv.at[0], (f, across))
    down_core = remote(down_ref, down_at(t), down_send.at[1], down_recv.at[1], (f, partner))
    down_here = pltpu.make_async_copy(down_ref, down_at(t), local_sem)
    down_cross.start()
    down_core.start()
    down_here.start()

    for c, p, j, m in swaps:
        c.wait_recv()
        start, size = (second, rest)[p]
        to_owner(stage_ref, across * blocks + j, j, m, p, start, size)

    native = (f // blocks) // 2 == plane
    near = jnp.where(native, 0, single)
    far = single - near

    def for_core(body):
        for m in range(mats):
            pl.when(core == m)(functools.partial(body, outs[m]))

    def arrive(p, order):
        def body(ref):
            for k in order:
                source = lax.rem(f + k, fs_count)
                start, size = (near, single) if p == 0 else (rest[0], rest[1])
                here = place(ref, source, start, size)
                remote(here, here, out_send.at[0], out_recv.at[source, p], (f, partner)).wait_recv()
                remote(
                    here, here, core_send.at[source, p], core_recv.at[source, p], (f, partner)
                ).start()
                if p == 0:
                    remote(
                        here, here, cross_send.at[source], cross_recv.at[source], (f, across)
                    ).start()
        return body

    for_core(arrive(0, range(fs_count)))

    down_in = remote(down_ref, down_at(across), down_send.at[0], down_recv.at[0], (f, across))
    down_in.wait_recv()
    down_on = remote(
        down_at(across), down_at(across), down_send.at[2], down_recv.at[2], (f, partner)
    )
    down_on.start()

    for_core(arrive(1, range(fs_count)))

    def last(ref):
        for k in range(fs_count):
            source = lax.rem(f + k, fs_count)
            here = place(ref, source, far, single)
            remote(
                here, here, cross_send.at[source], cross_recv.at[source], (f, across)
            ).wait_recv()
            remote(
                here, here, last_send.at[source], last_recv.at[source], (f, partner)
            ).start()

    for_core(last)

    def finish(mine, other):
        for source in range(fs_count):
            for p, (start, size) in enumerate(((near, single), rest)):
                a, b = place(mine, source, start, size), place(other, source, start, size)
                remote(
                    a, b, core_send.at[source, p], core_recv.at[source, p], (f, partner)
                ).wait()
            a, b = place(mine, source, far, single), place(other, source, far, single)
            remote(a, a, cross_send.at[source], cross_recv.at[source], (f, across)).wait_send()
            remote(a, b, last_send.at[source], last_recv.at[source], (f, partner)).wait()

    for m in range(mats):
        pl.when(core == m)(functools.partial(finish, outs[m], outs[1 - m]))
    for c, *_ in swaps:
        c.wait_send()
    for c, local in sends:
        pl.when(jnp.logical_not(local))(c.wait_send)
    down_here.wait()
    down_cross.wait_send()
    down_core.wait_send()
    remote(down_ref, down_at(partner), down_send.at[1], down_recv.at[1], (f, partner)).wait_recv()
    far_partner = plane * -2 + 2 + 1 - core
    down_on.wait_send()
    remote(
        down_ref, down_at(far_partner), down_send.at[2], down_recv.at[2], (f, partner)
    ).wait_recv()


def spread(fs_count, tp_count, src, down_local):
    blocks, mats, rows, cols = src.shape
    single = max(16, (rows * 5 // 32) // 16 * 16)
    ff_rows, down_cols = down_local.shape
    dma = pltpu.SemaphoreType.DMA
    bf16 = jnp.bfloat16
    count = 2 * blocks * mats
    any_spec = pl.BlockSpec(memory_space=pl.ANY)
    vmem_spec = pl.BlockSpec(memory_space=pltpu.VMEM)
    return pl.pallas_call(
        functools.partial(spread_kernel, fs_count, tp_count, single),
        out_shape=(
            jax.ShapeDtypeStruct((rows * fs_count, cols), bf16),
            jax.ShapeDtypeStruct((rows * fs_count, cols), bf16),
            jax.ShapeDtypeStruct((ff_rows, down_cols * tp_count), bf16),
        ),
        in_specs=[vmem_spec, vmem_spec],
        out_specs=(any_spec, any_spec, any_spec),
        scratch_shapes=[
            pltpu.VMEM((blocks, mats, rows, cols), bf16),
            dma((count,)), dma((count,)),
            dma((2 * count,)), dma((fs_count, 2)),
            dma((fs_count, 2)), dma((fs_count, 2)),
            dma((fs_count,)), dma((fs_count,)),
            dma((fs_count,)), dma((fs_count,)),
            dma((3,)), dma((3,)),
            dma(()),
        ],
        compiler_params=pltpu.CompilerParams(
            has_side_effects=True, vmem_limit_bytes=48 * 1024 * 1024
        ),
    )(src, down_local)


def scatter_sum(terms, fs_count):
    me = lax.axis_index("fs")
    width = terms.shape[1] // fs_count

    def part(which):
        return lax.dynamic_slice_in_dim(terms, which * width, width, axis=1)

    arrived = []
    for k in range(1, fs_count):
        ring = [(i, (i + k) % fs_count) for i in range(fs_count)]
        sent = part(lax.rem(me + k, fs_count)).astype(jnp.bfloat16)
        arrived.append(lax.ppermute(sent, "fs", ring))
    total = part(me)
    for piece in arrived:
        total = total + piece.astype(jnp.float32)
    return total.astype(jnp.bfloat16)


def per_device(tokens, norm_gain, gate_trained, up_trained, down_trained):
    tp_count = lax.axis_size("tp")
    fs_count = lax.axis_size("fs")
    rows_local, cols_local = gate_trained.shape
    owned_count = cols_local * tp_count // fs_count
    blocks = cols_local // owned_count

    def rounded(matrix, j):
        piece = matrix[:, j * owned_count:(j + 1) * owned_count]
        return (norm_gain[:, None] * piece).astype(jnp.bfloat16)

    src = jnp.stack(
        [jnp.stack([rounded(gate_trained, j), rounded(up_trained, j)]) for j in range(blocks)]
    )
    gate_sampler, up_sampler, down_sampler = spread(
        fs_count, tp_count, src, down_trained.astype(jnp.bfloat16)
    )
    as_float = tokens.astype(jnp.float32)
    normed = (
        as_float * lax.rsqrt(jnp.mean(as_float * as_float, axis=-1, keepdims=True) + 1e-06)
    ).astype(jnp.bfloat16)
    gate_act = jnp.dot(normed, gate_sampler, preferred_element_type=jnp.float32)
    up_act = jnp.dot(normed, up_sampler, preferred_element_type=jnp.float32)
    hidden = (jax.nn.silu(gate_act) * up_act).astype(jnp.bfloat16)
    terms = jnp.dot(hidden, down_sampler, preferred_element_type=jnp.float32)
    return (gate_sampler, up_sampler, down_sampler, scatter_sum(terms, fs_count))


def per_device_plain(tokens, norm_gain, gate_trained, up_trained, down_trained):
    gate_local = (norm_gain[:, None] * gate_trained).astype(jnp.bfloat16)
    up_local = (norm_gain[:, None] * up_trained).astype(jnp.bfloat16)
    down_local = down_trained.astype(jnp.bfloat16)
    tp_count = lax.axis_size("tp")
    fs_count = lax.axis_size("fs")
    rows_local = gate_local.shape[0]
    cols_local = gate_local.shape[1]
    model_width = rows_local * fs_count
    owned_count = cols_local * tp_count // fs_count
    piece_cols = owned_count // tp_count
    block_count = cols_local // owned_count

    def arrange(matrix):
        return matrix.reshape(rows_local, block_count, tp_count, piece_cols)

    gate_mixed, up_mixed = (
        lax.all_to_all(arrange(gate_local), "tp", split_axis=2, concat_axis=2, tiled=True),
        lax.all_to_all(arrange(up_local), "tp", split_axis=2, concat_axis=2, tiled=True),
    )

    def regroup(matrix):
        return matrix.transpose(2, 1, 0, 3).reshape(fs_count, rows_local, piece_cols)

    gate_parts, up_parts = (
        lax.all_to_all(regroup(gate_mixed), "fs", split_axis=0, concat_axis=1, tiled=True),
        lax.all_to_all(regroup(up_mixed), "fs", split_axis=0, concat_axis=1, tiled=True),
    )
    gate_sampler, up_sampler, down_sampler = (
        lax.all_gather(gate_parts.reshape(model_width, piece_cols), "tp", axis=1, tiled=True),
        lax.all_gather(up_parts.reshape(model_width, piece_cols), "tp", axis=1, tiled=True),
        lax.all_gather(down_local, "tp", axis=1, tiled=True),
    )
    as_float = tokens.astype(jnp.float32)
    normed = (
        as_float * lax.rsqrt(jnp.mean(as_float * as_float, axis=-1, keepdims=True) + 1e-06)
    ).astype(jnp.bfloat16)
    gate_act = jnp.dot(normed, gate_sampler, preferred_element_type=jnp.float32)
    up_act = jnp.dot(normed, up_sampler, preferred_element_type=jnp.float32)
    hidden = (jax.nn.silu(gate_act) * up_act).astype(jnp.bfloat16)
    partial_terms = jnp.dot(hidden, down_sampler, preferred_element_type=jnp.float32)
    mixed_out = lax.psum_scatter(partial_terms, "fs", scatter_dimension=1, tiled=True).astype(
        jnp.bfloat16
    )
    return (gate_sampler, up_sampler, down_sampler, mixed_out)


def solution(mesh):
    fs_count, tp_count = mesh.shape["fs"], mesh.shape["tp"]

    def body(tokens, norm_gain, gate_trained, up_trained, down_trained):
        rows, cols = gate_trained.shape
        aligned = (
            tp_count == 4
            and fs_count % tp_count == 0
            and rows % 16 == 0
            and rows >= 64
            and (cols * tp_count // fs_count) % 128 == 0
            and down_trained.shape[1] % 128 == 0
            and down_trained.shape[0] % 16 == 0
        )
        run = per_device if aligned else per_device_plain
        return run(tokens, norm_gain, gate_trained, up_trained, down_trained)

    in_specs = (P("tp", None), P("fs"), P("fs", "tp"), P("fs", "tp"), P("fs", "tp"))
    out_specs = (P(None, "fs"), P(None, "fs"), P("fs", None), P("tp", "fs"))
    return jax.shard_map(
        body, mesh=mesh, in_specs=in_specs, out_specs=out_specs, check_vma=False
    )
```

```python
import functools

import jax
import jax.numpy as jnp
from jax import lax
from jax.experimental import pallas as pl
from jax.experimental.pallas import tpu as pltpu
from jax.sharding import PartitionSpec as P

MESH = pl.DeviceIdType.MESH


def spread_kernel(
    fs_count, blocks, mats, single, *refs,
):
    src_refs, refs = refs[:blocks * mats], refs[blocks * mats:]
    spread_body(fs_count, blocks, mats, single, src_refs, *refs)


def spread_body(
    fs_count, blocks, mats, single, src_refs, down_ref, gate_ref, up_ref, down_out_ref, stage_ref,
    swap_send, swap_recv, out_send, out_recv, core_send, core_recv, cross_send, cross_recv,
    last_send, last_recv, down_send, down_recv, local_sem,
):
    rows = src_refs[0].shape[0]
    down_cols = down_ref.shape[1]
    f = lax.axis_index("fs")
    t = lax.axis_index("tp")
    plane, core = t // 2, t % 2
    across = plane * -2 + 2 + core
    partner = plane * 2 + 1 - core
    outs = (gate_ref, up_ref)
    pieces = ((0, single), (single, single), (2 * single, rows - 2 * single))
    first, second, rest = pieces

    def remote(src, dst, send, recv, to):
        return pltpu.make_async_remote_copy(
            src_ref=src, dst_ref=dst, send_sem=send, recv_sem=recv, device_id=to, device_id_type=MESH
        )

    def place(ref, source, start, size):
        return ref.at[pl.ds(pl.multiple_of(source * rows + start, 16), size), :]

    swaps = []
    for p, (start, size) in enumerate((second, rest)):
        for j in range(blocks):
            for m in range(mats):
                k = (p * blocks + j) * mats + m
                cut = pl.ds(start, size)
                c = remote(
                    src_refs[j * mats + m].at[cut, :], stage_ref.at[j, m, cut, :],
                    swap_send.at[k], swap_recv.at[k], (f, across),
                )
                c.start()
                swaps.append((c, p, j, m))

    sends = []

    def to_owner(ref, owner, j, m, p, start, size):
        k = len(sends)
        source = ref.at[pl.ds(start, size), :]
        landing = place(outs[m], f, start, size)
        local = jnp.logical_and(owner == f, core == m)
        there = remote(source, landing, out_send.at[k], out_recv.at[f, p], (owner, plane * 2 + m))

        @pl.when(local)
        def _():
            pltpu.make_async_copy(source, landing, out_recv.at[f, p]).start()

        @pl.when(jnp.logical_not(local))
        def _():
            there.start()

        sends.append((there, local))

    for p, (start, size) in enumerate((first, rest)):
        for j in range(blocks):
            for m in range(mats):
                to_owner(src_refs[j * mats + m], t * blocks + j, j, m, p, start, size)

    def down_at(which):
        return down_out_ref.at[:, pl.ds(pl.multiple_of(which * down_cols, 128), down_cols)]

    down_cross = remote(down_ref, down_at(t), down_send.at[0], down_recv.at[0], (f, across))
    down_core = remote(down_ref, down_at(t), down_send.at[1], down_recv.at[1], (f, partner))
    down_here = pltpu.make_async_copy(down_ref, down_at(t), local_sem)
    down_cross.start()
    down_core.start()
    down_here.start()

    for c, p, j, m in swaps:
        c.wait_recv()
        start, size = (second, rest)[p]
        to_owner(stage_ref.at[j, m], across * blocks + j, j, m, p, start, size)

    native = (f // blocks) // 2 == plane
    near = jnp.where(native, 0, single)
    far = single - near

    def for_core(body):
        for m in range(mats):
            pl.when(core == m)(functools.partial(body, outs[m]))

    def arrive(p, order):
        def body(ref):
            for k in order:
                source = lax.rem(f + k, fs_count)
                start, size = (near, single) if p == 0 else (rest[0], rest[1])
                here = place(ref, source, start, size)
                remote(here, here, out_send.at[0], out_recv.at[source, p], (f, partner)).wait_recv()
                remote(
                    here, here, core_send.at[source, p], core_recv.at[source, p], (f, partner)
                ).start()
                if p == 0:
                    remote(
                        here, here, cross_send.at[source], cross_recv.at[source], (f, across)
                    ).start()
        return body

    for_core(arrive(0, range(fs_count)))

    down_in = remote(down_ref, down_at(across), down_send.at[0], down_recv.at[0], (f, across))
    down_in.wait_recv()
    down_on = remote(
        down_at(across), down_at(across), down_send.at[2], down_recv.at[2], (f, partner)
    )
    down_on.start()

    for_core(arrive(1, range(fs_count)))

    def last(ref):
        for k in range(fs_count):
            source = lax.rem(f + k, fs_count)
            here = place(ref, source, far, single)
            remote(
                here, here, cross_send.at[source], cross_recv.at[source], (f, across)
            ).wait_recv()
            remote(
                here, here, last_send.at[source], last_recv.at[source], (f, partner)
            ).start()

    for_core(last)

    def finish(mine, other):
        for source in range(fs_count):
            for p, (start, size) in enumerate(((near, single), rest)):
                a, b = place(mine, source, start, size), place(other, source, start, size)
                remote(
                    a, b, core_send.at[source, p], core_recv.at[source, p], (f, partner)
                ).wait()
            a, b = place(mine, source, far, single), place(other, source, far, single)
            remote(a, a, cross_send.at[source], cross_recv.at[source], (f, across)).wait_send()
            remote(a, b, last_send.at[source], last_recv.at[source], (f, partner)).wait()

    for m in range(mats):
        pl.when(core == m)(functools.partial(finish, outs[m], outs[1 - m]))
    for c, *_ in swaps:
        c.wait_send()
    for c, local in sends:
        pl.when(jnp.logical_not(local))(c.wait_send)
    down_here.wait()
    down_cross.wait_send()
    down_core.wait_send()
    remote(down_ref, down_at(partner), down_send.at[1], down_recv.at[1], (f, partner)).wait_recv()
    far_partner = plane * -2 + 2 + 1 - core
    down_on.wait_send()
    remote(
        down_ref, down_at(far_partner), down_send.at[2], down_recv.at[2], (f, partner)
    ).wait_recv()


def spread(fs_count, tp_count, mats, srcs, down_local):
    rows, cols = srcs[0].shape
    blocks = len(srcs) // mats
    single = max(16, (rows * 5 // 32) // 16 * 16)
    ff_rows, down_cols = down_local.shape
    dma = pltpu.SemaphoreType.DMA
    bf16 = jnp.bfloat16
    count = 2 * blocks * mats
    any_spec = pl.BlockSpec(memory_space=pl.ANY)
    vmem_spec = pl.BlockSpec(memory_space=pltpu.VMEM)
    return pl.pallas_call(
        functools.partial(spread_kernel, fs_count, blocks, mats, single),
        out_shape=(
            jax.ShapeDtypeStruct((rows * fs_count, cols), bf16),
            jax.ShapeDtypeStruct((rows * fs_count, cols), bf16),
            jax.ShapeDtypeStruct((ff_rows, down_cols * tp_count), bf16),
        ),
        in_specs=[vmem_spec] * (blocks * mats + 1),
        out_specs=(any_spec, any_spec, any_spec),
        scratch_shapes=[
            pltpu.VMEM((blocks, mats, rows, cols), bf16),
            dma((count,)), dma((count,)),
            dma((2 * count,)), dma((fs_count, 2)),
            dma((fs_count, 2)), dma((fs_count, 2)),
            dma((fs_count,)), dma((fs_count,)),
            dma((fs_count,)), dma((fs_count,)),
            dma((3,)), dma((3,)),
            dma(()),
        ],
        compiler_params=pltpu.CompilerParams(
            has_side_effects=True, vmem_limit_bytes=48 * 1024 * 1024
        ),
    )(*srcs, down_local)


def put_out(landed):
    rows, cols = landed.shape
    step = max(r for r in range(16, min(rows, 512) + 1, 16) if rows % r == 0)

    def copy_kernel(in_ref, out_ref):
        out_ref[...] = in_ref[...]

    spec = pl.BlockSpec((step, cols), lambda i: (i, 0))
    return pl.pallas_call(
        copy_kernel,
        grid=(rows // step,),
        out_shape=jax.ShapeDtypeStruct(landed.shape, landed.dtype),
        in_specs=[spec],
        out_specs=spec,
        cost_estimate=pl.CostEstimate(
            flops=0, bytes_accessed=2 * landed.size * landed.dtype.itemsize, transcendentals=0
        ),
    )(landed)


def scatter_sum(terms, fs_count):
    me = lax.axis_index("fs")
    width = terms.shape[1] // fs_count

    def part(which):
        return lax.dynamic_slice_in_dim(terms, which * width, width, axis=1)

    arrived = []
    for k in range(1, fs_count):
        ring = [(i, (i + k) % fs_count) for i in range(fs_count)]
        sent = part(lax.rem(me + k, fs_count)).astype(jnp.bfloat16)
        arrived.append(lax.ppermute(sent, "fs", ring))
    total = part(me)
    for piece in arrived:
        total = total + piece.astype(jnp.float32)
    return total.astype(jnp.bfloat16)


def per_device(tokens, norm_gain, gate_trained, up_trained, down_trained):
    tp_count = lax.axis_size("tp")
    fs_count = lax.axis_size("fs")
    rows_local, cols_local = gate_trained.shape
    owned_count = cols_local * tp_count // fs_count
    blocks = cols_local // owned_count

    def rounded(matrix, j):
        piece = matrix[:, j * owned_count:(j + 1) * owned_count]
        return (norm_gain[:, None] * piece).astype(jnp.bfloat16)

    srcs = [rounded(matrix, j) for j in range(blocks) for matrix in (gate_trained, up_trained)]
    gate_sampler, up_sampler, down_sampler = spread(
        fs_count, tp_count, 2, srcs, down_trained.astype(jnp.bfloat16)
    )
    as_float = tokens.astype(jnp.float32)
    normed = (
        as_float * lax.rsqrt(jnp.mean(as_float * as_float, axis=-1, keepdims=True) + 1e-06)
    ).astype(jnp.bfloat16)
    gate_act = jnp.dot(normed, gate_sampler, preferred_element_type=jnp.float32)
    up_act = jnp.dot(normed, up_sampler, preferred_element_type=jnp.float32)
    hidden = (jax.nn.silu(gate_act) * up_act).astype(jnp.bfloat16)
    terms = jnp.dot(hidden, down_sampler, preferred_element_type=jnp.float32)
    gate_sampler, up_sampler, down_sampler, terms = lax.optimization_barrier(
        (gate_sampler, up_sampler, down_sampler, terms)
    )
    return (
        put_out(gate_sampler), put_out(up_sampler), put_out(down_sampler),
        scatter_sum(terms, fs_count),
    )


def per_device_plain(tokens, norm_gain, gate_trained, up_trained, down_trained):
    gate_local = (norm_gain[:, None] * gate_trained).astype(jnp.bfloat16)
    up_local = (norm_gain[:, None] * up_trained).astype(jnp.bfloat16)
    down_local = down_trained.astype(jnp.bfloat16)
    tp_count = lax.axis_size("tp")
    fs_count = lax.axis_size("fs")
    rows_local = gate_local.shape[0]
    cols_local = gate_local.shape[1]
    model_width = rows_local * fs_count
    owned_count = cols_local * tp_count // fs_count
    piece_cols = owned_count // tp_count
    block_count = cols_local // owned_count

    def arrange(matrix):
        return matrix.reshape(rows_local, block_count, tp_count, piece_cols)

    gate_mixed, up_mixed = (
        lax.all_to_all(arrange(gate_local), "tp", split_axis=2, concat_axis=2, tiled=True),
        lax.all_to_all(arrange(up_local), "tp", split_axis=2, concat_axis=2, tiled=True),
    )

    def regroup(matrix):
        return matrix.transpose(2, 1, 0, 3).reshape(fs_count, rows_local, piece_cols)

    gate_parts, up_parts = (
        lax.all_to_all(regroup(gate_mixed), "fs", split_axis=0, concat_axis=1, tiled=True),
        lax.all_to_all(regroup(up_mixed), "fs", split_axis=0, concat_axis=1, tiled=True),
    )
    gate_sampler, up_sampler, down_sampler = (
        lax.all_gather(gate_parts.reshape(model_width, piece_cols), "tp", axis=1, tiled=True),
        lax.all_gather(up_parts.reshape(model_width, piece_cols), "tp", axis=1, tiled=True),
        lax.all_gather(down_local, "tp", axis=1, tiled=True),
    )
    as_float = tokens.astype(jnp.float32)
    normed = (
        as_float * lax.rsqrt(jnp.mean(as_float * as_float, axis=-1, keepdims=True) + 1e-06)
    ).astype(jnp.bfloat16)
    gate_act = jnp.dot(normed, gate_sampler, preferred_element_type=jnp.float32)
    up_act = jnp.dot(normed, up_sampler, preferred_element_type=jnp.float32)
    hidden = (jax.nn.silu(gate_act) * up_act).astype(jnp.bfloat16)
    partial_terms = jnp.dot(hidden, down_sampler, preferred_element_type=jnp.float32)
    mixed_out = lax.psum_scatter(partial_terms, "fs", scatter_dimension=1, tiled=True).astype(
        jnp.bfloat16
    )
    return (gate_sampler, up_sampler, down_sampler, mixed_out)


def solution(mesh):
    fs_count, tp_count = mesh.shape["fs"], mesh.shape["tp"]

    def body(tokens, norm_gain, gate_trained, up_trained, down_trained):
        rows, cols = gate_trained.shape
        aligned = (
            tp_count == 4
            and fs_count % tp_count == 0
            and rows % 16 == 0
            and rows >= 64
            and (cols * tp_count // fs_count) % 128 == 0
            and down_trained.shape[1] % 128 == 0
            and down_trained.shape[0] % 16 == 0
        )
        run = per_device if aligned else per_device_plain
        return run(tokens, norm_gain, gate_trained, up_trained, down_trained)

    in_specs = (P("tp", None), P("fs"), P("fs", "tp"), P("fs", "tp"), P("fs", "tp"))
    out_specs = (P(None, "fs"), P(None, "fs"), P("fs", None), P("tp", "fs"))
    return jax.shard_map(
        body, mesh=mesh, in_specs=in_specs, out_specs=out_specs, check_vma=False
    )
```
